128 devices in a mesh: fs: 16 (over z, x), tp: 8 (over y, core).
Axes of the slice: x: 4, y: 4, z: 4, core: 2. Of those that a mesh axis runs over, the one named last changes fastest.
Arguments:
- normed_input: bfloat16 [32768, 2048], P('fs'), may hold values from -6 to 6
- forget_cot: bfloat16 [32768, 2048], P('fs', 'tp'), may hold values from -6 to 6
- value_cot: bfloat16 [32768, 2048], P('fs', 'tp'), may hold values from -6 to 6
- gated_output: bfloat16 [32768, 2048], P('fs', 'tp'), may hold values from -6 to 6
- output_cot: bfloat16 [32768, 2048], P('fs'), may hold values from -6 to 6
- forget_weight: float32 [2048, 2048], P('fs', 'tp'), may hold values from -0.125 to 0.125
- value_weight: float32 [2048, 2048], P('fs', 'tp'), may hold values from -0.125 to 0.125
- out_weight: float32 [2048, 2048], P('tp', 'fs'), may hold values from -0.125 to 0.125
- bases: bfloat16 [3, 2048, 256], replicated, may hold values from -0.125 to 0.125
- first_moment: float32 [256, 3, 2048], P('fs', None, 'tp'), may hold values from -4 to 4
- second_moment: float32 [256, 3, 2048], P('fs', None, 'tp'), may hold values from 0.25 to 4
Outputs:
- new_forget: float32 [2048, 2048], P('fs', 'tp')
- new_value: float32 [2048, 2048], P('fs', 'tp')
- new_out: float32 [2048, 2048], P('tp', 'fs')
- copy_forget: bfloat16 [2048, 2048], P(None, 'tp')
- copy_value: bfloat16 [2048, 2048], P(None, 'tp')
- copy_out: bfloat16 [2048, 2048], P('tp')
- moment_one: float32 [256, 3, 2048], P('fs', None, 'tp')
- moment_two: float32 [256, 3, 2048], P('fs', None, 'tp')
- step_forget: float32 [2048, 2048], P('fs', 'tp')
- step_value: float32 [2048, 2048], P('fs', 'tp')
- step_out: float32 [2048, 2048], P('tp', 'fs')
The draws below stay inside these ranges and needn't reach their ends.
All inputs are finite; a program needn't handle non-finite values.
Results may differ from the reference program's by a relative error of at most 0.0045.
Values may be sent and summed in bfloat16 or wider, within the bound.
A program may use at most 128 MiB of HBM per device.

```python
import math
import jax
import jax.numpy as jnp
from jax import lax

D = 2048
QK = 2048
V = 2048
RANK = 256
TOKENS = 32768


def draw_first_moment(key, part):
    base = jax.random.normal(key, (RANK, 3, QK), jnp.float32) * 0.5
    return jnp.clip(base, -4.0, 4.0)


def level_of(rng, dims, shards, smallest, top_value):
    gain = 1.0
    for dim, shards_of in shards:
        heights = jax.random.uniform(jax.random.fold_in(jax.random.fold_in(rng, 6), dim), (shards_of,), jnp.float32, smallest / len(shards), top_value / len(shards))
        gain = gain * jnp.repeat(jnp.exp(heights), dims[dim] // shards_of).reshape((-1,) + (1,) * (len(dims) - 1 - dim))
    return gain


def normal_values(rng, extent, spread, reach, shards=(), dtype=jnp.bfloat16):
    values = spread * jax.random.normal(rng, extent, jnp.float32)
    if shards:
        values = values * level_of(rng, extent, shards, -0.22, 0.18)
    return jnp.clip(values, -reach, reach).astype(dtype)


def setup_inputs(seed: int = 0) -> dict:
    arg_keys = jax.random.split(jax.random.key(seed), 12)
    normed_input = normal_values(arg_keys[0], (TOKENS, D), 1.0, 6.0, ((0, 16),))
    forget_cot = normal_values(arg_keys[1], (TOKENS, QK), 1.0, 6.0, ((0, 16), (1, 8)))
    value_cot = normal_values(arg_keys[2], (TOKENS, V), 1.0, 6.0, ((0, 16), (1, 8)))
    gated_output = normal_values(arg_keys[3], (TOKENS, V), 1.0, 6.0, ((0, 16), (1, 8)))
    output_cot = normal_values(arg_keys[4], (TOKENS, D), 1.0, 6.0, ((0, 16),))
    forget_weight = normal_values(arg_keys[5], (D, QK), D ** -0.5, 0.125, ((0, 16), (1, 8)), jnp.float32)
    value_weight = normal_values(arg_keys[6], (D, V), D ** -0.5, 0.125, ((0, 16), (1, 8)), jnp.float32)
    out_weight = normal_values(arg_keys[7], (V, D), V ** -0.5, 0.125, ((0, 8), (1, 16)), jnp.float32)
    bases = normal_values(arg_keys[8], (3, D, RANK), D ** -0.5, 0.125)
    first_moment = draw_first_moment(jax.random.fold_in(arg_keys[11], 71), 0)
    second_moment = jnp.clip(jnp.exp(math.log(4.0) - 2.7725887 * jax.random.uniform(arg_keys[10], (RANK, 3, QK), jnp.float32) ** level_of(arg_keys[10], (RANK, 3, QK), ((0, 16), (2, 8)), -0.2, 0.2)), 0.25, 4.0)
    return {"normed_input": normed_input, "forget_cot": forget_cot, "value_cot": value_cot, "gated_output": gated_output, "output_cot": output_cot, "forget_weight": forget_weight, "value_weight": value_weight, "out_weight": out_weight, "bases": bases, "first_moment": first_moment, "second_moment": second_moment}


def reference(normed_input, forget_cot, value_cot, gated_output, output_cot, forget_weight, value_weight, out_weight, bases, first_moment, second_moment):
    factor = float(TOKENS) ** (-0.5)
    grad_forget = jnp.dot(normed_input.T, forget_cot, preferred_element_type=jnp.float32) * factor
    grad_value = jnp.dot(normed_input.T, value_cot, preferred_element_type=jnp.float32) * factor
    grad_out = jnp.dot(output_cot.T, gated_output, preferred_element_type=jnp.float32) * factor
    grads = jnp.stack([grad_forget, grad_value, grad_out], axis=1)
    basis_full = bases.astype(jnp.float32)
    projected = jnp.einsum('kdr,dkc->rkc', basis_full, grads, precision=lax.Precision.HIGHEST)
    moment_one = 0.9 * first_moment + 0.1 * projected
    moment_two = 0.9 * second_moment + 0.1 * projected * projected
    direction = moment_one / (jnp.sqrt(moment_two) + 1e-08)
    scale = lax.rsqrt(lax.optimization_barrier(jnp.mean(direction * direction, axis=(0, 2))) + 1.0)
    full = jnp.einsum('kdr,rkc->dkc', basis_full, direction, precision=lax.Precision.HIGHEST)
    full = full * scale[None, :, None]
    step_forget = full[:, 0, :]
    step_value = full[:, 1, :]
    step_out = full[:, 2, :].T
    new_forget = forget_weight - 0.01 * step_forget
    new_value = value_weight - 0.01 * step_value
    new_out = out_weight - 0.01 * step_out
    return (new_forget, new_value, new_out, new_forget.astype(jnp.bfloat16), new_value.astype(jnp.bfloat16), new_out.astype(jnp.bfloat16), moment_one, moment_two, step_forget, step_value, step_out)
```

```python
import functools

import jax
import jax.numpy as jnp
from jax import lax
from jax.experimental import pallas as pl
from jax.experimental.pallas import tpu as pltpu
from jax.sharding import Mesh
from jax.sharding import PartitionSpec as P

FS = ("z", "x")
TP = ("y", "c")
F32 = jnp.float32
BF16 = jnp.bfloat16
RING = 4
PEERS = [(dz, dx) for dz in range(4) for dx in range(4) if (dz, dx) != (0, 0)]
TP_PEERS = [(dy, dc) for dy in range(4) for dc in range(2) if (dy, dc) != (0, 0)]
CHUNK = 256
MiB = 1 << 20


def contract(lhs, rhs, left, right):
    return lax.dot_general(lhs, rhs, (((left,), (right,)), ((), ())), preferred_element_type=F32)


def exchange(
    x_hbm, y_hbm, fc_hbm, vc_hbm, go_hbm, wf_hbm, wv_hbm, wo_hbm, b_hbm, m1_hbm, m2_hbm,
    g, dg, tot, m1o, m2o, bcat, wf, wv, wo,
    xb, yb, cots, m1b, m2b, pacc, psend, parr, s1, s2,
    wsem, bsem, msem, xsem, ysem, csem, gs, gr, a_s, a_r, d_s, d_r, t_s, t_r, u_s, u_r,
):
    at = {a: lax.axis_index(a) for a in ("z", "x", "y", "c")}
    shift = lambda a, d: lax.rem(at[a] + (d % RING), RING)
    me = at["z"] * RING + at["x"]
    tokens = xb.shape[0]
    chunks = tokens // CHUNK
    factor = float(tokens * RING * RING) ** (-0.5)

    w_copies = [
        pltpu.make_async_copy(s, d, wsem.at[i])
        for i, (s, d) in enumerate(((wf_hbm, wf), (wv_hbm, wv), (wo_hbm, wo)))
    ]
    b_copies = [
        pltpu.make_async_copy(b_hbm.at[k], bcat.at[:, 256 * k : 256 * k + 256], bsem.at[k])
        for k in range(3)
    ]
    m_copies = [
        pltpu.make_async_copy(s, d, msem.at[i]) for i, (s, d) in enumerate(((m1_hbm, m1b), (m2_hbm, m2b)))
    ]

    def rows_of(i):
        return pl.ds(pl.multiple_of(i * CHUNK, CHUNK), CHUNK)

    def x_copies(i):
        r = rows_of(i)
        return (
            pltpu.make_async_copy(x_hbm.at[r], xb.at[r], xsem.at[i]),
            pltpu.make_async_copy(fc_hbm.at[r], cots.at[0, r], csem.at[0, i]),
            pltpu.make_async_copy(vc_hbm.at[r], cots.at[1, r], csem.at[1, i]),
        )

    def y_copies(i):
        r = rows_of(i)
        return (
            pltpu.make_async_copy(y_hbm.at[r], yb.at[r], ysem.at[i]),
            pltpu.make_async_copy(go_hbm.at[r], cots.at[2, r], csem.at[2, i]),
        )

    for c in w_copies:
        c.start()
    b_copies[0].start()
    b_copies[1].start()

    @pl.loop(0, chunks)
    def _(i):
        for c in x_copies(i):
            c.start()

    b_copies[2].start()

    @pl.loop(0, chunks)
    def _(i):
        for c in y_copies(i):
            c.start()

    for c in m_copies:
        c.start()

    barrier = pltpu.get_barrier_semaphore()
    plane = [{"z": shift("z", dz), "x": shift("x", dx)} for dz, dx in PEERS]
    heads = [{"y": shift("y", dy), "c": lax.rem(at["c"] + dc, 2)} for dy, dc in TP_PEERS]
    for peer in plane + heads:
        pl.semaphore_signal(barrier, inc=1, device_id=peer)

    for c in w_copies:
        c.wait()
    for p in range(2):
        lanes = slice(128 * p, 128 * p + 128)
        g[me, 128 * p : 128 * p + 128, :] = wf[:, lanes].astype(BF16)
        g[me, 256 + 128 * p : 384 + 128 * p, :] = wv[:, lanes].astype(BF16)
    g[me, 512:768, :] = wo[...].astype(BF16)
    pacc[...] = jnp.zeros_like(pacc)
    pl.semaphore_wait(barrier, len(PEERS) + len(TP_PEERS))

    half, quarter = 384, 192

    def block(h, ja, jb):
        a, b = ("x", "z") if h == 0 else ("z", "x")
        pos = {a: shift(a, ja), b: shift(b, jb)}
        return pos["z"] * RING + pos["x"]

    def hop(h, n, ja, jb, sub, along, d):
        axis = ("x", "z")[h] if along == 0 else ("z", "x")[h]
        start, size = (half * h, half) if sub is None else (half * h + quarter * sub, quarter)

        def ref(a, b):
            return g.at[block(h, a, b), start : start + size]

        src = ref(ja, jb)
        came = ref(ja - d, jb) if along == 0 else ref(ja, jb - d)
        peer = {axis: shift(axis, d)}
        out = pltpu.make_async_remote_copy(src, src, gs.at[h, n], gr.at[h, n], device_id=peer)
        arriving = pltpu.make_async_remote_copy(came, came, gs.at[h, n], gr.at[h, n], device_id=peer)
        return out, arriving

    hops = []
    for h in range(2):
        hops.append(hop(h, 0, 0, 0, None, 0, 1))
        hops.append(hop(h, 1, 0, 0, None, 0, -1))
        hops.append(hop(h, 2, -1, 0, 0, 0, 1))
        hops.append(hop(h, 3, 1, 0, 1, 0, -1))
        for j, ja in enumerate((0, -1, 1, 2)):
            hops.append(hop(h, 4 + 4 * j, ja, 0, None, 1, 1))
            hops.append(hop(h, 5 + 4 * j, ja, 0, None, 1, -1))
            hops.append(hop(h, 6 + 4 * j, ja, -1, 0, 1, 1))
            hops.append(hop(h, 7 + 4 * j, ja, 1, 1, 1, -1))

    def send(*ids):
        for n in ids:
            for h in range(2):
                hops[20 * h + n][0].start()

    def arrive(*ids):
        for n in ids:
            for h in range(2):
                hops[20 * h + n][1].wait_recv()

    send(0, 1, 4, 5)

    b_copies[0].wait()
    b_copies[1].wait()

    def x_chunk(i):
        for c in x_copies(i):
            c.wait()
        r = rows_of(i)
        red = jnp.dot(xb[r, :], bcat[:, 0:512], preferred_element_type=F32).astype(BF16)
        pacc[0] += contract(red[:, :256], cots[0, r], 0, 0)
        pacc[1] += contract(red[:, 256:], cots[1, r], 0, 0)

    def y_chunk(i):
        for c in y_copies(i):
            c.wait()
        r = rows_of(i)
        red = jnp.dot(yb[r, :], bcat[:, 512:768], preferred_element_type=F32).astype(BF16)
        pacc[2] += contract(red, cots[2, r], 0, 0)

    pl.loop(0, chunks // 2)(x_chunk)
    pl.loop(chunks // 2, chunks)(x_chunk)
    arrive(0, 1)
    send(2, 3, 8, 9, 12, 13)

    def to_owners(ks, n):
        copies = []
        for slot, ((dz, dx), peer) in enumerate(zip(PEERS, plane)):
            owner = peer["z"] * RING + peer["x"]
            r = pl.ds(pl.multiple_of(owner * 16, 16), 16)
            copies.append(
                pltpu.make_async_remote_copy(
                    psend.at[ks, r, :], parr.at[ks, slot], a_s.at[n, slot], a_r.at[n, slot], device_id=peer
                )
            )
        return copies

    psend[0:2] = (pacc[0:2] * factor).astype(BF16)
    first = to_owners(slice(0, 2), 0)
    for c in first:
        c.start()

    b_copies[2].wait()
    pl.loop(0, chunks)(y_chunk)
    psend[2] = (pacc[2] * factor).astype(BF16)
    second = to_owners(slice(2, 3), 1)
    for c in second:
        c.start()

    arrive(4, 5)
    send(6, 7)
    arrive(2, 3)
    send(16, 17)

    for c in m_copies:
        c.wait()
    for c in first + second:
        c.wait_recv()
    mine = pl.ds(pl.multiple_of(me * 16, 16), 16)
    sums = []
    for k in range(3):
        total = psend[k, mine, :].astype(F32)
        for slot in range(len(PEERS)):
            total = total + parr[k, slot].astype(F32)
        first_moment = 0.9 * m1b[k] + 0.1 * total
        second_moment = 0.9 * m2b[k] + 0.1 * total * total
        direction = first_moment / (jnp.sqrt(second_moment) + 1e-08)
        m1o[k] = first_moment
        m2o[k] = second_moment
        dg[k, mine, :] = direction.astype(BF16)
        sums.append(jnp.sum(direction * direction))
    lane = lax.broadcasted_iota(jnp.int32, (1, 128), 1)
    row = jnp.zeros((1, 128), F32)
    for k in range(3):
        row = row + jnp.where(lane == k, sums[k], 0.0)
    s1[len(TP_PEERS)] = row
    across = [
        pltpu.make_async_remote_copy(
            s1.at[len(TP_PEERS)], s1.at[n], t_s.at[n], t_r.at[n], device_id=peer
        )
        for n, peer in enumerate(heads)
    ]
    for c in across:
        c.start()
    spread = [
        pltpu.make_async_remote_copy(
            dg.at[:, mine, :], dg.at[:, mine, :], d_s.at[n], d_r.at[n], device_id=peer
        )
        for n, peer in enumerate(plane)
    ]
    for c in spread:
        c.start()
    for c in across:
        c.wait_recv()
    s2[len(PEERS)] = jnp.sum(s1[...], axis=0)
    around = [
        pltpu.make_async_remote_copy(
            s2.at[len(PEERS)], s2.at[n], u_s.at[n], u_r.at[n], device_id=peer
        )
        for n, peer in enumerate(plane)
    ]
    for c in around:
        c.start()

    arrive(8, 9, 12, 13)
    send(10, 11, 14, 15)
    arrive(16, 17)
    send(18, 19)

    for n, ((dz, dx), peer) in enumerate(zip(PEERS, plane)):
        came = shift("z", -dz) * RING + shift("x", -dx)
        r = pl.ds(pl.multiple_of(came * 16, 16), 16)
        pltpu.make_async_remote_copy(
            dg.at[:, r, :], dg.at[:, r, :], d_s.at[n], d_r.at[n], device_id=peer
        ).wait_recv()
    for c in around:
        c.wait_recv()
    tot[...] = jnp.sum(s2[...], axis=0)
    arrive(6, 7, 10, 11, 14, 15, 18, 19)
    for out, _ in hops:
        out.wait_send()
    for c in first + second + across + spread + around:
        c.wait_send()


def finish(
    entries, g, dg, tot, m1i, m2i, bcat, wf, wv, wo,
    nf_h, nv_h, no_h, cf_h, cv_h, co_h, m1_h, m2_h, sf_h, sv_h, so_h,
    nf, nv, no, cf, cv, co, sf, sv, so, dt, sem, csem,
):
    me = lax.axis_index("z") * RING + lax.axis_index("x")
    moments = [
        pltpu.make_async_copy(m1i, m1_h, sem.at[0]),
        pltpu.make_async_copy(m2i, m2_h, sem.at[1]),
    ]
    for c in moments:
        c.start()
    row = tot[...]
    lane = lax.broadcasted_iota(jnp.int32, (1, 128), 1)
    scale = [
        lax.rsqrt(jnp.sum(jnp.where(lane == k, row, 0.0), axis=1, keepdims=True) / entries + 1.0)
        for k in range(3)
    ]
    dt[...] = dg[2].astype(F32).T.astype(BF16)
    rows = pl.ds(pl.multiple_of(me * 128, 128), 128)
    for k, (w, new, step) in enumerate(((wf, nf, sf), (wv, nv, sv))):
        full = jnp.dot(bcat[rows, 256 * k : 256 * k + 256], dg[k], preferred_element_type=F32) * scale[k]
        step[...] = full
        new[...] = w[...] - 0.01 * full
    full = contract(dt[...], bcat[rows, 512:768], 1, 1) * scale[2]
    so[...] = full
    no[...] = wo[...] - 0.01 * full
    own = [
        pltpu.make_async_copy(s, d, sem.at[2 + i])
        for i, (s, d) in enumerate(
            ((nf, nf_h), (nv, nv_h), (no, no_h), (sf, sf_h), (sv, sv_h), (so, so_h))
        )
    ]
    for c in own:
        c.start()
    outs = []
    for i in range(8):
        r = slice(256 * i, 256 * i + 256)
        for k, (copy, hbm) in enumerate(((cf, cf_h), (cv, cv_h))):
            full = jnp.dot(bcat[r, 256 * k : 256 * k + 256], dg[k], preferred_element_type=F32)
            full = full * (0.01 * scale[k])
            for b in range(2):
                for p in range(2):
                    base = 256 * k + 128 * p
                    old = g[2 * i + b, base : base + 128, :].astype(F32)
                    part = full[128 * b : 128 * b + 128, 128 * p : 128 * p + 128]
                    copy[256 * i + 128 * b : 256 * i + 128 * b + 128, 128 * p : 128 * p + 128] = (
                        old - part
                    ).astype(BF16)
            outs.append(pltpu.make_async_copy(copy.at[r], hbm.at[r], csem.at[k, i]))
            outs[-1].start()
        full = contract(dt[...], bcat[r, 512:768], 1, 1) * (0.01 * scale[2])
        for b in range(2):
            old = g[2 * i + b, 512:768, :].astype(F32)
            co[:, 256 * i + 128 * b : 256 * i + 128 * b + 128] = (
                old - full[:, 128 * b : 128 * b + 128]
            ).astype(BF16)
        outs.append(pltpu.make_async_copy(co.at[:, r], co_h.at[:, r], csem.at[2, i]))
        outs[-1].start()
    for c in moments + own + outs:
        c.wait()


def on_device(x, fc, vc, go, y, wf, wv, wo, bases, m1, m2):
    tokens = x.shape[0]
    hbm = pl.BlockSpec(memory_space=pltpu.HBM)
    vmem = pl.BlockSpec(memory_space=pltpu.VMEM)
    dma = pltpu.SemaphoreType.DMA
    m1, m2 = (jnp.transpose(m, (1, 0, 2)) for m in (m1, m2))
    args = [
        pltpu.with_memory_space_constraint(a, pltpu.HBM) for a in (x, y, fc, vc, go, wf, wv, wo, bases, m1, m2)
    ]
    held = pl.pallas_call(
        exchange,
        name="exchange",
        out_shape=[
            pltpu.VMEM((16, 768, 128), BF16),
            pltpu.VMEM((3, 256, 256), BF16),
            pltpu.VMEM((1, 128), F32),
            pltpu.VMEM((3, 16, 256), F32),
            pltpu.VMEM((3, 16, 256), F32),
            pltpu.VMEM((2048, 768), BF16),
            pltpu.VMEM((128, 256), F32),
            pltpu.VMEM((128, 256), F32),
            pltpu.VMEM((256, 128), F32),
        ],
        in_specs=[hbm] * 11,
        out_specs=[vmem] * 9,
        scratch_shapes=[
            pltpu.VMEM((tokens, 2048), BF16),
            pltpu.VMEM((tokens, 2048), BF16),
            pltpu.VMEM((3, tokens, 256), BF16),
            pltpu.VMEM((3, 16, 256), F32),
            pltpu.VMEM((3, 16, 256), F32),
            pltpu.VMEM((3, 256, 256), F32),
            pltpu.VMEM((3, 256, 256), BF16),
            pltpu.VMEM((3, 15, 16, 256), BF16),
            pltpu.VMEM((8, 1, 128), F32),
            pltpu.VMEM((16, 1, 128), F32),
            dma((3,)),
            dma((3,)),
            dma((2,)),
            dma((8,)),
            dma((8,)),
            dma((3, 8)),
            dma((2, 20)),
            dma((2, 20)),
            dma((2, 15)),
            dma((2, 15)),
            dma((15,)),
            dma((15,)),
            dma((7,)),
            dma((7,)),
            dma((15,)),
            dma((15,)),
        ],
        compiler_params=pltpu.CompilerParams(
            collective_id=0, has_side_effects=True, vmem_limit_bytes=40 * MiB
        ),
    )(*args)
    shapes = [
        ((128, 256), F32),
        ((128, 256), F32),
        ((256, 128), F32),
        ((2048, 256), BF16),
        ((2048, 256), BF16),
        ((256, 2048), BF16),
        ((3, 16, 256), F32),
        ((3, 16, 256), F32),
        ((128, 256), F32),
        ((128, 256), F32),
        ((256, 128), F32),
    ]
    outs = pl.pallas_call(
        functools.partial(finish, float(256 * 2048)),
        name="finish",
        out_shape=[jax.ShapeDtypeStruct(*s) for s in shapes],
        in_specs=[vmem] * 9,
        out_specs=[hbm] * 11,
        scratch_shapes=[
            *(pltpu.VMEM(*s) for s in shapes[:6]),
            *(pltpu.VMEM(*s) for s in shapes[8:]),
            pltpu.VMEM((256, 256), BF16),
            dma((8,)),
            dma((3, 8)),
        ],
        compiler_params=pltpu.CompilerParams(vmem_limit_bytes=24 * MiB),
    )(*held)
    outs = list(outs)
    outs[6], outs[7] = (jnp.transpose(m, (1, 0, 2)) for m in outs[6:8])
    return tuple(outs)


def solution(mesh):
    torus = Mesh(mesh.devices.reshape(4, 4, 4, 2), ("z", "x", "y", "c"))
    rows, heads, both = P(FS, None), P(FS, TP), P(FS, None, TP)
    turned = P(TP, FS)
    return jax.shard_map(
        on_device,
        mesh=torus,
        in_specs=(rows, heads, heads, heads, rows, heads, heads, turned, P(), both, both),
        out_specs=(
            heads, heads, turned, P(None, TP), P(None, TP), P(TP, None), both, both, heads, heads, turned,
        ),
        check_vma=False,
    )
```

```python
import functools

import jax
import jax.numpy as jnp
from jax import lax
from jax.experimental import pallas as pl
from jax.experimental.pallas import tpu as pltpu
from jax.sharding import Mesh
from jax.sharding import PartitionSpec as P

FS = ("z", "x")
TP = ("y", "c")
F32 = jnp.float32
BF16 = jnp.bfloat16
RING = 4
HOPS = (1, 2, 3)
PEERS = [(dz, dx) for dz in range(4) for dx in range(4) if (dz, dx) != (0, 0)]
AXES = (("x", "z"), ("z", "x"))
TP_PEERS = [(dy, dc) for dy in range(4) for dc in range(2) if (dy, dc) != (0, 0)]
CHUNK = 512
MiB = 1 << 20


def contract(lhs, rhs, left, right):
    return lax.dot_general(lhs, rhs, (((left,), (right,)), ((), ())), preferred_element_type=F32)


def exchange(
    x_hbm, y_hbm, fc_hbm, vc_hbm, go_hbm, wf_hbm, wv_hbm, wo_hbm, b_hbm, m1_hbm, m2_hbm,
    g, dg, tot, m1o, m2o, bcat, wf, wv, wo,
    xb, yb, cots, red, m1b, m2b, pacc, psend, parr, s1, s2,
    wsem, bsem, msem, xsem, ysem, csem, r_s, r_r, gs, gr, a_s, a_r, d_s, d_r, e_s, e_r, t_s, t_r, u_s, u_r,
):
    at = {a: lax.axis_index(a) for a in ("z", "x", "y", "c")}
    shift = lambda a, d: lax.rem(at[a] + (d % RING), RING)
    me = at["z"] * RING + at["x"]
    half_tokens = xb.shape[0]
    tokens = 2 * half_tokens
    chunks = half_tokens // CHUNK
    factor = float(tokens * RING * RING) ** (-0.5)
    mine_from = at["c"] * half_tokens
    other_from = half_tokens - mine_from

    w_copies = [
        pltpu.make_async_copy(s, d, wsem.at[i])
        for i, (s, d) in enumerate(((wf_hbm, wf), (wv_hbm, wv), (wo_hbm, wo)))
    ]
    b_copies = [
        pltpu.make_async_copy(b_hbm.at[k], bcat.at[:, 256 * k : 256 * k + 256], bsem.at[k])
        for k in range(3)
    ]
    m_copies = [
        pltpu.make_async_copy(s, d, msem.at[i]) for i, (s, d) in enumerate(((m1_hbm, m1b), (m2_hbm, m2b)))
    ]

    def in_array(i):
        return pl.ds(pl.multiple_of(mine_from + i * CHUNK, CHUNK), CHUNK)

    def in_half(i):
        return slice(i * CHUNK, i * CHUNK + CHUNK)

    x_copies = [
        pltpu.make_async_copy(x_hbm.at[in_array(i)], xb.at[in_half(i)], xsem.at[i]) for i in range(chunks)
    ]
    y_copies = [
        pltpu.make_async_copy(y_hbm.at[in_array(i)], yb.at[in_half(i)], ysem.at[i]) for i in range(chunks)
    ]
    c_copies = [
        pltpu.make_async_copy(s, cots.at[k], csem.at[k]) for k, s in enumerate((fc_hbm, vc_hbm, go_hbm))
    ]

    barrier = pltpu.get_barrier_semaphore()
    plane = [{"z": shift("z", dz), "x": shift("x", dx)} for dz, dx in PEERS]
    ring = {a: [{a: shift(a, d)} for d in HOPS] for a in ("x", "z")}
    heads = [{"y": shift("y", dy), "c": lax.rem(at["c"] + dc, 2)} for dy, dc in TP_PEERS]
    for peer in plane + heads:
        pl.semaphore_signal(barrier, inc=1, device_id=peer)

    for c in w_copies + b_copies[:2] + x_copies:
        c.start()
    for c in w_copies:
        c.wait()
    for p in range(2):
        lanes = slice(128 * p, 128 * p + 128)
        g[me, 128 * p : 128 * p + 128, :] = wf[:, lanes].astype(BF16)
        g[me, 256 + 128 * p : 384 + 128 * p, :] = wv[:, lanes].astype(BF16)
    g[me, 512:768, :] = wo[...].astype(BF16)
    pl.semaphore_wait(barrier, len(PEERS) + len(TP_PEERS))

    def reduce_x(i):
        red[in_array(i), 0:512] = jnp.dot(
            xb[in_half(i), :], bcat[:, 0:512], preferred_element_type=F32
        ).astype(BF16)

    def reduce_y(i):
        red[in_array(i), 512:768] = jnp.dot(
            yb[in_half(i), :], bcat[:, 512:768], preferred_element_type=F32
        ).astype(BF16)

    mine_rows = pl.ds(pl.multiple_of(mine_from, CHUNK), half_tokens)
    other_rows = pl.ds(pl.multiple_of(other_from, CHUNK), half_tokens)
    partner = {"c": 1 - at["c"]}

    def shared(rows, lanes, n):
        ref = red.at[rows, lanes]
        return pltpu.make_async_remote_copy(ref, ref, r_s.at[n], r_r.at[n], device_id=partner)

    x_part, y_part = slice(0, 512), slice(512, 768)
    in_other = [pl.ds(pl.multiple_of(other_from + i * CHUNK, CHUNK), CHUNK) for i in range(chunks)]
    over, back = (
        [shared(part(i), lanes, chunks * n + i) for n, lanes in enumerate((x_part, y_part)) for i in range(chunks)]
        for part in (in_array, lambda i: in_other[i])
    )

    def project(k, rows):
        return contract(red[rows, 256 * k : 256 * k + 256], cots[k, rows], 0, 0)

    half, quarter = 384, 192

    def block(h, ja, jb):
        a, b = ("x", "z") if h == 0 else ("z", "x")
        pos = {a: shift(a, ja), b: shift(b, jb)}
        return pos["z"] * RING + pos["x"]

    def hop(h, n, ja, jb, sub, along, d):
        axis = ("x", "z")[h] if along == 0 else ("z", "x")[h]
        start, size = (half * h, half) if sub is None else (half * h + quarter * sub, quarter)

        def ref(a, b):
            return g.at[block(h, a, b), start : start + size]

        src = ref(ja, jb)
        came = ref(ja - d, jb) if along == 0 else ref(ja, jb - d)
        peer = {axis: shift(axis, d)}
        out = pltpu.make_async_remote_copy(src, src, gs.at[h, n], gr.at[h, n], device_id=peer)
        arriving = pltpu.make_async_remote_copy(came, came, gs.at[h, n], gr.at[h, n], device_id=peer)
        return out, arriving

    hops = []
    for h in range(2):
        hops.append(hop(h, 0, 0, 0, None, 0, 1))
        hops.append(hop(h, 1, 0, 0, None, 0, -1))
        hops.append(hop(h, 2, -1, 0, 0, 0, 1))
        hops.append(hop(h, 3, 1, 0, 1, 0, -1))
        for j, ja in enumerate((0, -1, 1, 2)):
            hops.append(hop(h, 4 + 4 * j, ja, 0, None, 1, 1))
            hops.append(hop(h, 5 + 4 * j, ja, 0, None, 1, -1))
            hops.append(hop(h, 6 + 4 * j, ja, -1, 0, 1, 1))
            hops.append(hop(h, 7 + 4 * j, ja, 1, 1, 1, -1))

    def send(*ids):
        for n in ids:
            for h in range(2):
                hops[20 * h + n][0].start()

    def arrive(*ids):
        for n in ids:
            for h in range(2):
                hops[20 * h + n][1].wait_recv()

    send(0, 1, 4, 5)

    for c in b_copies[:2]:
        c.wait()
    x_copies[0].wait()
    for c in b_copies[2:] + y_copies + c_copies + m_copies:
        c.start()
    reduce_x(0)
    over[0].start()
    x_copies[1].wait()
    reduce_x(1)
    over[1].start()

    for c in c_copies[:2]:
        c.wait()
    for k in range(2):
        pacc[k] = project(k, mine_rows)

    def to_owners(ks, n):
        copies = []
        for slot, peer in enumerate(plane):
            owner = peer["z"] * RING + peer["x"]
            r = pl.ds(pl.multiple_of(owner * 16, 16), 16)
            copies.append(
                pltpu.make_async_remote_copy(
                    psend.at[ks, r, :], parr.at[ks, slot], a_s.at[n, slot], a_r.at[n, slot], device_id=peer
                )
            )
        return copies

    back[0].wait_recv()
    back[1].wait_recv()
    for k in range(2):
        psend[k] = ((pacc[k] + project(k, other_rows)) * factor).astype(BF16)
    first = to_owners(slice(0, 2), 0)
    for c in first:
        c.start()

    b_copies[2].wait()
    y_copies[0].wait()
    reduce_y(0)
    over[2].start()
    y_copies[1].wait()
    reduce_y(1)
    over[3].start()
    c_copies[2].wait()
    pacc[2] = project(2, mine_rows)
    arrive(0, 1)
    send(2, 3)
    back[2].wait_recv()
    back[3].wait_recv()
    psend[2] = ((pacc[2] + project(2, other_rows)) * factor).astype(BF16)
    second = to_owners(slice(2, 3), 1)
    for c in second:
        c.start()

    send(8, 9, 12, 13)
    for c in m_copies:
        c.wait()
    for c in first + second:
        c.wait_recv()
    mine = pl.ds(pl.multiple_of(me * 16, 16), 16)
    squares = []
    for k in range(3):
        total = psend[k, mine, :].astype(F32)
        for slot in range(len(PEERS)):
            total = total + parr[k, slot].astype(F32)
        first_moment = 0.9 * m1b[k] + 0.1 * total
        second_moment = 0.9 * m2b[k] + 0.1 * total * total
        direction = first_moment / (jnp.sqrt(second_moment) + 1e-08)
        m1o[k] = first_moment
        m2o[k] = second_moment
        for h in range(2):
            dg[h, k, at["z"], at["x"]] = direction[:, 128 * h : 128 * h + 128].astype(BF16)
        squares.append(direction * direction)

    def spread_copies(h, axis, where, sems):
        copies, arriving = [], []
        for i, (d, peer) in enumerate(zip(HOPS, ring[axis])):
            src, came = where(at[axis]), where(shift(axis, -d))
            copies.append(
                pltpu.make_async_remote_copy(src, src, sems[0].at[h, i], sems[1].at[h, i], device_id=peer)
            )
            arriving.append(
                pltpu.make_async_remote_copy(came, came, sems[0].at[h, i], sems[1].at[h, i], device_id=peer)
            )
        return copies, arriving

    near = [
        spread_copies(0, "x", lambda x: dg.at[0, :, at["z"], x], (d_s, d_r)),
        spread_copies(1, "z", lambda z: dg.at[1, :, z, at["x"]], (d_s, d_r)),
    ]
    far = [
        spread_copies(0, "z", lambda z: dg.at[0, :, z], (e_s, e_r)),
        spread_copies(1, "x", lambda x: dg.at[1, :, :, x], (e_s, e_r)),
    ]
    for copies, _ in near:
        for c in copies:
            c.start()

    sums = [jnp.sum(v) for v in squares]
    lane = lax.broadcasted_iota(jnp.int32, (1, 128), 1)
    row = jnp.zeros((1, 128), F32)
    for k in range(3):
        row = row + jnp.where(lane == k, sums[k], 0.0)

    def sum_copies(held, peers, send_sems, recv_sems):
        return [
            pltpu.make_async_remote_copy(
                held.at[len(peers)], held.at[n], send_sems.at[n], recv_sems.at[n], device_id=peer
            )
            for n, peer in enumerate(peers)
        ]

    across = sum_copies(s1, heads, t_s, t_r)
    around = sum_copies(s2, plane, u_s, u_r)
    s1[len(TP_PEERS)] = row
    for c in across:
        c.start()

    arrive(4, 5)
    send(6, 7)
    arrive(2, 3)
    send(16, 17)

    for c in across:
        c.wait_recv()
    s2[len(PEERS)] = jnp.sum(s1[...], axis=0)
    for c in around:
        c.start()
    for _, arriving in near:
        for c in arriving:
            c.wait_recv()
    for copies, _ in far:
        for c in copies:
            c.start()

    arrive(8, 9, 12, 13)
    send(10, 11, 14, 15)
    arrive(16, 17)
    send(18, 19)

    for _, arriving in far:
        for c in arriving:
            c.wait_recv()
    for c in around:
        c.wait_recv()
    tot[...] = jnp.sum(s2[...], axis=0)
    arrive(6, 7, 10, 11, 14, 15, 18, 19)
    for out, _ in hops:
        out.wait_send()
    sent = over + first + second + across + around
    for copies, _ in near + far:
        sent = sent + copies
    for c in sent:
        c.wait_send()


def finish(
    entries, g, dg, tot, m1i, m2i, bcat, wf, wv, wo,
    nf_h, nv_h, no_h, cf_h, cv_h, co_h, m1_h, m2_h, sf_h, sv_h, so_h,
    nf, nv, no, cf, cv, co, sf, sv, so, dirs, dt, sem, csem,
):
    me = lax.axis_index("z") * RING + lax.axis_index("x")
    moments = [
        pltpu.make_async_copy(m1i, m1_h, sem.at[0]),
        pltpu.make_async_copy(m2i, m2_h, sem.at[1]),
    ]
    for c in moments:
        c.start()
    row = tot[...]
    lane = lax.broadcasted_iota(jnp.int32, (1, 128), 1)
    scale = [
        lax.rsqrt(jnp.sum(jnp.where(lane == k, row, 0.0), axis=1, keepdims=True) / entries + 1.0)
        for k in range(3)
    ]
    for k in range(3):
        for h in range(2):
            dirs[k, :, 128 * h : 128 * h + 128] = dg[h, k].reshape(256, 128)
    dt[...] = dirs[2].astype(F32).T.astype(BF16)
    rows = pl.ds(pl.multiple_of(me * 128, 128), 128)
    for k, (w, new, step) in enumerate(((wf, nf, sf), (wv, nv, sv))):
        full = jnp.dot(bcat[rows, 256 * k : 256 * k + 256], dirs[k], preferred_element_type=F32) * scale[k]
        step[...] = full
        new[...] = w[...] - 0.01 * full
    full = contract(dt[...], bcat[rows, 512:768], 1, 1) * scale[2]
    so[...] = full
    no[...] = wo[...] - 0.01 * full
    own = [
        pltpu.make_async_copy(s, d, sem.at[2 + i])
        for i, (s, d) in enumerate(
            ((nf, nf_h), (nv, nv_h), (no, no_h), (sf, sf_h), (sv, sv_h), (so, so_h))
        )
    ]
    for c in own:
        c.start()
    outs = []
    for i in range(8):
        r = slice(256 * i, 256 * i + 256)
        for k, (copy, hbm) in enumerate(((cf, cf_h), (cv, cv_h))):
            full = jnp.dot(bcat[r, 256 * k : 256 * k + 256], dirs[k], preferred_element_type=F32)
            full = full * (0.01 * scale[k])
            for b in range(2):
                for p in range(2):
                    base = 256 * k + 128 * p
                    old = g[2 * i + b, base : base + 128, :].astype(F32)
                    part = full[128 * b : 128 * b + 128, 128 * p : 128 * p + 128]
                    copy[256 * i + 128 * b : 256 * i + 128 * b + 128, 128 * p : 128 * p + 128] = (
                        old - part
                    ).astype(BF16)
            outs.append(pltpu.make_async_copy(copy.at[r], hbm.at[r], csem.at[k, i]))
            outs[-1].start()
        full = contract(dt[...], bcat[r, 512:768], 1, 1) * (0.01 * scale[2])
        for b in range(2):
            old = g[2 * i + b, 512:768, :].astype(F32)
            co[:, 256 * i + 128 * b : 256 * i + 128 * b + 128] = (
                old - full[:, 128 * b : 128 * b + 128]
            ).astype(BF16)
        outs.append(pltpu.make_async_copy(co.at[:, r], co_h.at[:, r], csem.at[2, i]))
        outs[-1].start()
    for c in moments + own + outs:
        c.wait()


def on_device(x, fc, vc, go, y, wf, wv, wo, bases, m1, m2):
    tokens = x.shape[0]
    hbm = pl.BlockSpec(memory_space=pltpu.HBM)
    vmem = pl.BlockSpec(memory_space=pltpu.VMEM)
    dma = pltpu.SemaphoreType.DMA
    m1, m2 = (jnp.transpose(m, (1, 0, 2)) for m in (m1, m2))
    args = [
        pltpu.with_memory_space_constraint(a, pltpu.HBM) for a in (x, y, fc, vc, go, wf, wv, wo, bases, m1, m2)
    ]
    held = pl.pallas_call(
        exchange,
        name="exchange",
        out_shape=[
            pltpu.VMEM((16, 768, 128), BF16),
            pltpu.VMEM((2, 3, 4, 4, 16, 128), BF16),
            pltpu.VMEM((1, 128), F32),
            pltpu.VMEM((3, 16, 256), F32),
            pltpu.VMEM((3, 16, 256), F32),
            pltpu.VMEM((2048, 768), BF16),
            pltpu.VMEM((128, 256), F32),
            pltpu.VMEM((128, 256), F32),
            pltpu.VMEM((256, 128), F32),
        ],
        in_specs=[hbm] * 11,
        out_specs=[vmem] * 9,
        scratch_shapes=[
            pltpu.VMEM((tokens // 2, 2048), BF16),
            pltpu.VMEM((tokens // 2, 2048), BF16),
            pltpu.VMEM((3, tokens, 256), BF16),
            pltpu.VMEM((tokens, 768), BF16),
            pltpu.VMEM((3, 16, 256), F32),
            pltpu.VMEM((3, 16, 256), F32),
            pltpu.VMEM((3, 256, 256), F32),
            pltpu.VMEM((3, 256, 256), BF16),
            pltpu.VMEM((3, 15, 16, 256), BF16),
            pltpu.VMEM((8, 1, 128), F32),
            pltpu.VMEM((16, 1, 128), F32),
            dma((3,)),
            dma((3,)),
            dma((2,)),
            dma((2,)),
            dma((2,)),
            dma((3,)),
            dma((4,)),
            dma((4,)),
            dma((2, 20)),
            dma((2, 20)),
            dma((2, 15)),
            dma((2, 15)),
            dma((2, 3)),
            dma((2, 3)),
            dma((2, 3)),
            dma((2, 3)),
            dma((7,)),
            dma((7,)),
            dma((15,)),
            dma((15,)),
        ],
        compiler_params=pltpu.CompilerParams(
            collective_id=0, has_side_effects=True, vmem_limit_bytes=40 * MiB
        ),
    )(*args)
    shapes = [
        ((128, 256), F32),
        ((128, 256), F32),
        ((256, 128), F32),
        ((2048, 256), BF16),
        ((2048, 256), BF16),
        ((256, 2048), BF16),
        ((3, 16, 256), F32),
        ((3, 16, 256), F32),
        ((128, 256), F32),
        ((128, 256), F32),
        ((256, 128), F32),
    ]
    outs = pl.pallas_call(
        functools.partial(finish, float(256 * 2048)),
        name="finish",
        out_shape=[jax.ShapeDtypeStruct(*s) for s in shapes],
        in_specs=[vmem] * 9,
        out_specs=[hbm] * 11,
        scratch_shapes=[
            *(pltpu.VMEM(*s) for s in shapes[:6]),
            *(pltpu.VMEM(*s) for s in shapes[8:]),
            pltpu.VMEM((3, 256, 256), BF16),
            pltpu.VMEM((256, 256), BF16),
            dma((8,)),
            dma((3, 8)),
        ],
        compiler_params=pltpu.CompilerParams(vmem_limit_bytes=24 * MiB),
    )(*held)
    outs = list(outs)
    outs[6], outs[7] = (jnp.transpose(m, (1, 0, 2)) for m in outs[6:8])
    return tuple(outs)


def solution(mesh):
    torus = Mesh(mesh.devices.reshape(4, 4, 4, 2), ("z", "x", "y", "c"))
    rows, heads, both = P(FS, None), P(FS, TP), P(FS, None, TP)
    turned = P(TP, FS)
    return jax.shard_map(
        on_device,
        mesh=torus,
        in_specs=(rows, heads, heads, heads, rows, heads, heads, turned, P(), both, both),
        out_specs=(
            heads, heads, turned, P(None, TP), P(None, TP), P(TP, None), both, both, heads, heads, turned,
        ),
        check_vma=False,
    )
```

```python
import functools

import jax
import jax.numpy as jnp
from jax import lax
from jax.experimental import pallas as pl
from jax.experimental.pallas import tpu as pltpu
from jax.sharding import Mesh
from jax.sharding import PartitionSpec as P

FS = ("z", "x")
TP = ("y", "c")
F32 = jnp.float32
BF16 = jnp.bfloat16
RING = 4
HOPS = (1, 2, 3)
PEERS = [(dz, dx) for dz in (2, 1, 3, 0) for dx in (2, 1, 3, 0) if (dz, dx) != (0, 0)]
AXES = (("x", "z"), ("z", "x"))
TP_PEERS = [(dy, dc) for dy in (2, 1, 3, 0) for dc in (1, 0) if (dy, dc) != (0, 0)]
CHUNK = 512
MiB = 1 << 20


def contract(lhs, rhs, left, right):
    return lax.dot_general(lhs, rhs, (((left,), (right,)), ((), ())), preferred_element_type=F32)


def exchange(
    x_hbm, y_hbm, fc_hbm, vc_hbm, go_hbm, wf_hbm, wv_hbm, wo_hbm, b_hbm, m1_hbm, m2_hbm,
    g, dg, tot, m1o, m2o, bcat, wf, wv, wo,
    xb, yb, cots, red, m1b, m2b, pacc, psend, parr, s1, s2,
    wsem, bsem, msem, xsem, ysem, csem, r_s, r_r, gs, gr, a_s, a_r, d_s, d_r, e_s, e_r, t_s, t_r, u_s, u_r,
):
    at = {a: lax.axis_index(a) for a in ("z", "x", "y", "c")}
    shift = lambda a, d: lax.rem(at[a] + (d % RING), RING)
    me = at["z"] * RING + at["x"]
    half_tokens = xb.shape[0]
    tokens = 2 * half_tokens
    chunks = half_tokens // CHUNK
    factor = float(tokens * RING * RING) ** (-0.5)
    mine_from = at["c"] * half_tokens
    other_from = half_tokens - mine_from

    w_copies = [
        pltpu.make_async_copy(s, d, wsem.at[i])
        for i, (s, d) in enumerate(((wf_hbm, wf), (wv_hbm, wv), (wo_hbm, wo)))
    ]
    b_copies = [
        pltpu.make_async_copy(b_hbm.at[k], bcat.at[:, 256 * k : 256 * k + 256], bsem.at[k])
        for k in range(3)
    ]
    m_copies = [
        pltpu.make_async_copy(s, d, msem.at[i]) for i, (s, d) in enumerate(((m1_hbm, m1b), (m2_hbm, m2b)))
    ]

    def in_array(i):
        return pl.ds(pl.multiple_of(mine_from + i * CHUNK, CHUNK), CHUNK)

    def in_half(i):
        return slice(i * CHUNK, i * CHUNK + CHUNK)

    x_copies = [
        pltpu.make_async_copy(x_hbm.at[in_array(i)], xb.at[in_half(i)], xsem.at[i]) for i in range(chunks)
    ]
    y_copies = [
        pltpu.make_async_copy(y_hbm.at[in_array(i)], yb.at[in_half(i)], ysem.at[i]) for i in range(chunks)
    ]
    c_copies = [
        pltpu.make_async_copy(s, cots.at[k], csem.at[k]) for k, s in enumerate((fc_hbm, vc_hbm, go_hbm))
    ]

    for c in w_copies:
        c.start()
    barrier = pltpu.get_barrier_semaphore()
    plane = [{"z": shift("z", dz), "x": shift("x", dx)} for dz, dx in PEERS]
    ring = {a: [{a: shift(a, d)} for d in HOPS] for a in ("x", "z")}
    heads = [{"y": shift("y", dy), "c": lax.rem(at["c"] + dc, 2)} for dy, dc in TP_PEERS]
    for peer in plane + heads:
        pl.semaphore_signal(barrier, inc=1, device_id=peer)

    for c in b_copies[:2] + x_copies:
        c.start()
    for c in w_copies:
        c.wait()
    for p in range(2):
        lanes = slice(128 * p, 128 * p + 128)
        g[me, 128 * p : 128 * p + 128, :] = wf[:, lanes].astype(BF16)
        g[me, 256 + 128 * p : 384 + 128 * p, :] = wv[:, lanes].astype(BF16)
    g[me, 512:768, :] = wo[...].astype(BF16)
    pl.semaphore_wait(barrier, len(PEERS) + len(TP_PEERS))

    def reduce_x(i):
        red[in_array(i), 0:512] = jnp.dot(
            xb[in_half(i), :], bcat[:, 0:512], preferred_element_type=F32
        ).astype(BF16)

    mine_rows = pl.ds(pl.multiple_of(mine_from, CHUNK), half_tokens)
    other_rows = pl.ds(pl.multiple_of(other_from, CHUNK), half_tokens)
    partner = {"c": 1 - at["c"]}

    def shared(rows, lanes, n):
        ref = red.at[rows, lanes]
        return pltpu.make_async_remote_copy(ref, ref, r_s.at[n], r_r.at[n], device_id=partner)

    x_part, y_part = slice(0, 512), slice(512, 768)
    in_other = [pl.ds(pl.multiple_of(other_from + i * CHUNK, CHUNK), CHUNK) for i in range(chunks)]
    over, back = (
        [shared(part(i), lanes, chunks * n + i) for n, lanes in enumerate((x_part, y_part)) for i in range(chunks)]
        for part in (in_array, lambda i: in_other[i])
    )

    def project(k, rows):
        return contract(red[rows, 256 * k : 256 * k + 256], cots[k, rows], 0, 0)

    half, quarter = 384, 192

    def block(h, ja, jb):
        a, b = ("x", "z") if h == 0 else ("z", "x")
        pos = {a: shift(a, ja), b: shift(b, jb)}
        return pos["z"] * RING + pos["x"]

    def hop(h, n, ja, jb, sub, along, d):
        axis = ("x", "z")[h] if along == 0 else ("z", "x")[h]
        start, size = (half * h, half) if sub is None else (half * h + quarter * sub, quarter)

        def ref(a, b):
            return g.at[block(h, a, b), start : start + size]

        src = ref(ja, jb)
        came = ref(ja - d, jb) if along == 0 else ref(ja, jb - d)
        peer = {axis: shift(axis, d)}
        out = pltpu.make_async_remote_copy(src, src, gs.at[h, n], gr.at[h, n], device_id=peer)
        arriving = pltpu.make_async_remote_copy(came, came, gs.at[h, n], gr.at[h, n], device_id=peer)
        return out, arriving

    hops = []
    for h in range(2):
        hops.append(hop(h, 0, 0, 0, None, 0, 1))
        hops.append(hop(h, 1, 0, 0, None, 0, -1))
        hops.append(hop(h, 2, -1, 0, 0, 0, 1))
        hops.append(hop(h, 3, 1, 0, 1, 0, -1))
        for j, ja in enumerate((0, -1, 1, 2)):
            hops.append(hop(h, 4 + 4 * j, ja, 0, None, 1, 1))
            hops.append(hop(h, 5 + 4 * j, ja, 0, None, 1, -1))
            hops.append(hop(h, 6 + 4 * j, ja, -1, 0, 1, 1))
            hops.append(hop(h, 7 + 4 * j, ja, 1, 1, 1, -1))

    def send(*ids):
        for n in ids:
            for h in range(2):
                hops[20 * h + n][0].start()

    def arrive(*ids):
        for n in ids:
            for h in range(2):
                hops[20 * h + n][1].wait_recv()

    send(0, 1, 4, 5)

    for c in b_copies[:2]:
        c.wait()
    x_copies[0].wait()
    for c in b_copies[2:] + y_copies + c_copies + m_copies:
        c.start()
    reduce_x(0)
    over[0].start()
    x_copies[1].wait()
    reduce_x(1)
    over[1].start()

    for c in c_copies[:2]:
        c.wait()
    for k in range(2):
        pacc[k] = project(k, mine_rows)

    def to_owners(ks, n):
        copies = []
        for slot, peer in enumerate(plane):
            owner = peer["z"] * RING + peer["x"]
            r = pl.ds(pl.multiple_of(owner * 16, 16), 16)
            copies.append(
                pltpu.make_async_remote_copy(
                    psend.at[ks, r, :], parr.at[ks, slot], a_s.at[n, slot], a_r.at[n, slot], device_id=peer
                )
            )
        return copies

    back[0].wait_recv()
    back[1].wait_recv()
    for k in range(2):
        psend[k] = ((pacc[k] + project(k, other_rows)) * factor).astype(BF16)
    first = to_owners(slice(0, 2), 0)
    for c in first:
        c.start()

    b_copies[2].wait()
    for c in y_copies:
        c.wait()
    red[mine_rows, 512:768] = jnp.dot(yb[...], bcat[:, 512:768], preferred_element_type=F32).astype(BF16)
    over[2].start()
    over[3].start()
    c_copies[2].wait()
    pacc[2] = project(2, mine_rows)
    arrive(0, 1)
    send(2, 3)
    back[2].wait_recv()
    back[3].wait_recv()
    psend[2] = ((pacc[2] + project(2, other_rows)) * factor).astype(BF16)
    second = to_owners(slice(2, 3), 1)
    for c in second:
        c.start()

    send(8, 9, 12, 13)
    for c in m_copies:
        c.wait()
    for c in first + second:
        c.wait_recv()
    mine = pl.ds(pl.multiple_of(me * 16, 16), 16)
    squares = []
    for k in range(3):
        total = psend[k, mine, :].astype(F32)
        for slot in range(len(PEERS)):
            total = total + parr[k, slot].astype(F32)
        first_moment = 0.9 * m1b[k] + 0.1 * total
        second_moment = 0.9 * m2b[k] + 0.1 * total * total
        direction = first_moment / (jnp.sqrt(second_moment) + 1e-08)
        m1o[k] = first_moment
        m2o[k] = second_moment
        for h in range(2):
            dg[h, k, at["z"], at["x"]] = direction[:, 128 * h : 128 * h + 128].astype(BF16)
        squares.append(direction * direction)

    def spread_copies(h, axis, where, sems):
        copies, arriving = [], []
        for i, (d, peer) in enumerate(zip(HOPS, ring[axis])):
            src, came = where(at[axis]), where(shift(axis, -d))
            copies.append(
                pltpu.make_async_remote_copy(src, src, sems[0].at[h, i], sems[1].at[h, i], device_id=peer)
            )
            arriving.append(
                pltpu.make_async_remote_copy(came, came, sems[0].at[h, i], sems[1].at[h, i], device_id=peer)
            )
        return copies, arriving

    near = [
        spread_copies(0, "x", lambda x: dg.at[0, :, at["z"], x], (d_s, d_r)),
        spread_copies(1, "z", lambda z: dg.at[1, :, z, at["x"]], (d_s, d_r)),
    ]
    far = [
        spread_copies(0, "z", lambda z: dg.at[0, :, z], (e_s, e_r)),
        spread_copies(1, "x", lambda x: dg.at[1, :, :, x], (e_s, e_r)),
    ]
    for copies, _ in near:
        for c in copies:
            c.start()

    sums = [jnp.sum(v) for v in squares]
    lane = lax.broadcasted_iota(jnp.int32, (1, 128), 1)
    row = jnp.zeros((1, 128), F32)
    for k in range(3):
        row = row + jnp.where(lane == k, sums[k], 0.0)

    def sum_copies(held, peers, send_sems, recv_sems):
        return [
            pltpu.make_async_remote_copy(
                held.at[len(peers)], held.at[n], send_sems.at[n], recv_sems.at[n], device_id=peer
            )
            for n, peer in enumerate(peers)
        ]

    across = sum_copies(s1, heads, t_s, t_r)
    around = sum_copies(s2, plane, u_s, u_r)
    s1[len(TP_PEERS)] = row
    for c in across:
        c.start()

    arrive(2, 3)
    send(16, 17)
    arrive(4, 5)
    send(6, 7)

    for _, arriving in near:
        for c in arriving:
            c.wait_recv()
    for copies, _ in far:
        for c in copies:
            c.start()
    for c in across:
        c.wait_recv()
    s2[len(PEERS)] = jnp.sum(s1[...], axis=0)
    for c in around:
        c.start()

    arrive(8, 9, 12, 13)
    send(10, 11, 14, 15)
    arrive(16, 17)
    send(18, 19)

    for _, arriving in far:
        for c in arriving:
            c.wait_recv()
    for c in around:
        c.wait_recv()
    tot[...] = jnp.sum(s2[...], axis=0)
    arrive(6, 7, 10, 11, 14, 15, 18, 19)
    for out, _ in hops:
        out.wait_send()
    sent = over + first + second + across + around
    for copies, _ in near + far:
        sent = sent + copies
    for c in sent:
        c.wait_send()


def finish(
    entries, g, dg, tot, m1i, m2i, bcat, wf, wv, wo,
    nf_h, nv_h, no_h, cf_h, cv_h, co_h, m1_h, m2_h, sf_h, sv_h, so_h,
    nf, nv, no, cf, cv, co, sf, sv, so, dirs, dt, sem, csem,
):
    me = lax.axis_index("z") * RING + lax.axis_index("x")
    moments = [
        pltpu.make_async_copy(m1i, m1_h, sem.at[0]),
        pltpu.make_async_copy(m2i, m2_h, sem.at[1]),
    ]
    for c in moments:
        c.start()
    row = tot[...]
    lane = lax.broadcasted_iota(jnp.int32, (1, 128), 1)
    scale = [
        lax.rsqrt(jnp.sum(jnp.where(lane == k, row, 0.0), axis=1, keepdims=True) / entries + 1.0)
        for k in range(3)
    ]
    for k in range(3):
        for h in range(2):
            dirs[k, :, 128 * h : 128 * h + 128] = dg[h, k].reshape(256, 128)
    dt[...] = dirs[2].astype(F32).T.astype(BF16)
    rows = pl.ds(pl.multiple_of(me * 128, 128), 128)
    for k, (w, new, step) in enumerate(((wf, nf, sf), (wv, nv, sv))):
        full = jnp.dot(bcat[rows, 256 * k : 256 * k + 256], dirs[k], preferred_element_type=F32) * scale[k]
        step[...] = full
        new[...] = w[...] - 0.01 * full
    full = contract(dt[...], bcat[rows, 512:768], 1, 1) * scale[2]
    so[...] = full
    no[...] = wo[...] - 0.01 * full
    own = [
        pltpu.make_async_copy(s, d, sem.at[2 + i])
        for i, (s, d) in enumerate(
            ((nf, nf_h), (nv, nv_h), (no, no_h), (sf, sf_h), (sv, sv_h), (so, so_h))
        )
    ]
    for c in own:
        c.start()
    outs = []
    for i in range(8):
        r = slice(256 * i, 256 * i + 256)
        for k, (copy, hbm) in enumerate(((cf, cf_h), (cv, cv_h))):
            full = jnp.dot(bcat[r, 256 * k : 256 * k + 256], dirs[k], preferred_element_type=F32)
            full = full * (0.01 * scale[k])
            for b in range(2):
                for p in range(2):
                    base = 256 * k + 128 * p
                    old = g[2 * i + b, base : base + 128, :].astype(F32)
                    part = full[128 * b : 128 * b + 128, 128 * p : 128 * p + 128]
                    copy[256 * i + 128 * b : 256 * i + 128 * b + 128, 128 * p : 128 * p + 128] = (
                        old - part
                    ).astype(BF16)
            outs.append(pltpu.make_async_copy(copy.at[r], hbm.at[r], csem.at[k, i]))
            outs[-1].start()
        full = contract(dt[...], bcat[r, 512:768], 1, 1) * (0.01 * scale[2])
        for b in range(2):
            old = g[2 * i + b, 512:768, :].astype(F32)
            co[:, 256 * i + 128 * b : 256 * i + 128 * b + 128] = (
                old - full[:, 128 * b : 128 * b + 128]
            ).astype(BF16)
        outs.append(pltpu.make_async_copy(co.at[:, r], co_h.at[:, r], csem.at[2, i]))
        outs[-1].start()
    for c in moments + own + outs:
        c.wait()


def on_device(x, fc, vc, go, y, wf, wv, wo, bases, m1, m2):
    tokens = x.shape[0]
    hbm = pl.BlockSpec(memory_space=pltpu.HBM)
    vmem = pl.BlockSpec(memory_space=pltpu.VMEM)
    dma = pltpu.SemaphoreType.DMA
    m1, m2 = (jnp.transpose(m, (1, 0, 2)) for m in (m1, m2))
    args = [
        pltpu.with_memory_space_constraint(a, pltpu.HBM) for a in (x, y, fc, vc, go, wf, wv, wo, bases, m1, m2)
    ]
    held = pl.pallas_call(
        exchange,
        name="exchange",
        out_shape=[
            pltpu.VMEM((16, 768, 128), BF16),
            pltpu.VMEM((2, 3, 4, 4, 16, 128), BF16),
            pltpu.VMEM((1, 128), F32),
            pltpu.VMEM((3, 16, 256), F32),
            pltpu.VMEM((3, 16, 256), F32),
            pltpu.VMEM((2048, 768), BF16),
            pltpu.VMEM((128, 256), F32),
            pltpu.VMEM((128, 256), F32),
            pltpu.VMEM((256, 128), F32),
        ],
        in_specs=[hbm] * 11,
        out_specs=[vmem] * 9,
        scratch_shapes=[
            pltpu.VMEM((tokens // 2, 2048), BF16),
            pltpu.VMEM((tokens // 2, 2048), BF16),
            pltpu.VMEM((3, tokens, 256), BF16),
            pltpu.VMEM((tokens, 768), BF16),
            pltpu.VMEM((3, 16, 256), F32),
            pltpu.VMEM((3, 16, 256), F32),
            pltpu.VMEM((3, 256, 256), F32),
            pltpu.VMEM((3, 256, 256), BF16),
            pltpu.VMEM((3, 15, 16, 256), BF16),
            pltpu.VMEM((8, 1, 128), F32),
            pltpu.VMEM((16, 1, 128), F32),
            dma((3,)),
            dma((3,)),
            dma((2,)),
            dma((2,)),
            dma((2,)),
            dma((3,)),
            dma((4,)),
            dma((4,)),
            dma((2, 20)),
            dma((2, 20)),
            dma((2, 15)),
            dma((2, 15)),
            dma((2, 3)),
            dma((2, 3)),
            dma((2, 3)),
            dma((2, 3)),
            dma((7,)),
            dma((7,)),
            dma((15,)),
            dma((15,)),
        ],
        compiler_params=pltpu.CompilerParams(
            collective_id=0, has_side_effects=True, vmem_limit_bytes=40 * MiB
        ),
    )(*args)
    shapes = [
        ((128, 256), F32),
        ((128, 256), F32),
        ((256, 128), F32),
        ((2048, 256), BF16),
        ((2048, 256), BF16),
        ((256, 2048), BF16),
        ((3, 16, 256), F32),
        ((3, 16, 256), F32),
        ((128, 256), F32),
        ((128, 256), F32),
        ((256, 128), F32),
    ]
    outs = pl.pallas_call(
        functools.partial(finish, float(256 * 2048)),
        name="finish",
        out_shape=[jax.ShapeDtypeStruct(*s) for s in shapes],
        in_specs=[vmem] * 9,
        out_specs=[hbm] * 11,
        scratch_shapes=[
            *(pltpu.VMEM(*s) for s in shapes[:6]),
            *(pltpu.VMEM(*s) for s in shapes[8:]),
            pltpu.VMEM((3, 256, 256), BF16),
            pltpu.VMEM((256, 256), BF16),
            dma((8,)),
            dma((3, 8)),
        ],
        compiler_params=pltpu.CompilerParams(vmem_limit_bytes=24 * MiB),
    )(*held)
    outs = list(outs)
    outs[6], outs[7] = (jnp.transpose(m, (1, 0, 2)) for m in outs[6:8])
    return tuple(outs)


def solution(mesh):
    torus = Mesh(mesh.devices.reshape(4, 4, 4, 2), ("z", "x", "y", "c"))
    rows, heads, both = P(FS, None), P(FS, TP), P(FS, None, TP)
    turned = P(TP, FS)
    return jax.shard_map(
        on_device,
        mesh=torus,
        in_specs=(rows, heads, heads, heads, rows, heads, heads, turned, P(), both, both),
        out_specs=(
            heads, heads, turned, P(None, TP), P(None, TP), P(TP, None), both, both, heads, heads, turned,
        ),
        check_vma=False,
    )
```

```python
import functools

import jax
import jax.numpy as jnp
from jax import lax
from jax.experimental import pallas as pl
from jax.experimental.pallas import tpu as pltpu
from jax.sharding import Mesh
from jax.sharding import PartitionSpec as P

FS = ("z", "x")
TP = ("y", "c")
F32 = jnp.float32
BF16 = jnp.bfloat16
RING = 4
HOPS = (1, 2, 3)
PEERS = [(dz, dx) for dz in (2, 1, 3, 0) for dx in (2, 1, 3, 0) if (dz, dx) != (0, 0)]
AXES = (("x", "z"), ("z", "x"))
TP_PEERS = [(dy, dc) for dy in (2, 1, 3, 0) for dc in (1, 0) if (dy, dc) != (0, 0)]
CHUNK = 512
MiB = 1 << 20


def contract(lhs, rhs, left, right):
    return lax.dot_general(lhs, rhs, (((left,), (right,)), ((), ())), preferred_element_type=F32)


def exchange(
    x_hbm, y_hbm, fc_hbm, vc_hbm, go_hbm, wf_hbm, wv_hbm, wo_hbm, b_hbm, m1_hbm, m2_hbm,
    g, dg, tot, m1o, m2o, bcat, wf, wv, wo,
    xb, yb, cots, red, m1b, m2b, pacc, psend, parr, s1, s2,
    wsem, bsem, msem, xsem, ysem, csem, r_s, r_r, gs, gr, a_s, a_r, d_s, d_r, e_s, e_r, t_s, t_r, u_s, u_r,
):
    at = {a: lax.axis_index(a) for a in ("z", "x", "y", "c")}
    shift = lambda a, d: lax.rem(at[a] + (d % RING), RING)
    me = at["z"] * RING + at["x"]
    half_tokens = xb.shape[0]
    tokens = 2 * half_tokens
    chunks = half_tokens // CHUNK
    factor = float(tokens * RING * RING) ** (-0.5)
    mine_from = at["c"] * half_tokens
    other_from = half_tokens - mine_from

    w_copies = [
        pltpu.make_async_copy(s, d, wsem.at[i])
        for i, (s, d) in enumerate(((wf_hbm, wf), (wv_hbm, wv), (wo_hbm, wo)))
    ]
    b_copies = [
        pltpu.make_async_copy(b_hbm.at[k], bcat.at[:, 256 * k : 256 * k + 256], bsem.at[k])
        for k in range(3)
    ]
    m_copies = [
        pltpu.make_async_copy(s, d, msem.at[i]) for i, (s, d) in enumerate(((m1_hbm, m1b), (m2_hbm, m2b)))
    ]

    def in_array(i):
        return pl.ds(pl.multiple_of(mine_from + i * CHUNK, CHUNK), CHUNK)

    def in_half(i):
        return slice(i * CHUNK, i * CHUNK + CHUNK)

    x_copies = [
        pltpu.make_async_copy(x_hbm.at[in_array(i)], xb.at[in_half(i)], xsem.at[i]) for i in range(chunks)
    ]
    y_copies = [
        pltpu.make_async_copy(y_hbm.at[in_array(i)], yb.at[in_half(i)], ysem.at[i]) for i in range(chunks)
    ]
    c_copies = [
        pltpu.make_async_copy(s, cots.at[k], csem.at[k]) for k, s in enumerate((fc_hbm, vc_hbm, go_hbm))
    ]

    for c in w_copies:
        c.start()
    barrier = pltpu.get_barrier_semaphore()
    plane = [{"z": shift("z", dz), "x": shift("x", dx)} for dz, dx in PEERS]
    ring = {a: [{a: shift(a, d)} for d in HOPS] for a in ("x", "z")}
    heads = [{"y": shift("y", dy), "c": lax.rem(at["c"] + dc, 2)} for dy, dc in TP_PEERS]
    for peer in plane + heads:
        pl.semaphore_signal(barrier, inc=1, device_id=peer)

    for c in b_copies[:2] + x_copies:
        c.start()
    for c in w_copies:
        c.wait()
    for p in range(2):
        lanes = slice(128 * p, 128 * p + 128)
        g[me, 128 * p : 128 * p + 128, :] = wf[:, lanes].astype(BF16)
        g[me, 256 + 128 * p : 384 + 128 * p, :] = wv[:, lanes].astype(BF16)
    g[me, 512:768, :] = wo[...].astype(BF16)
    pl.semaphore_wait(barrier, len(PEERS) + len(TP_PEERS))

    def reduce_x(i):
        red[in_array(i), 0:512] = jnp.dot(
            xb[in_half(i), :], bcat[:, 0:512], preferred_element_type=F32
        ).astype(BF16)

    mine_rows = pl.ds(pl.multiple_of(mine_from, CHUNK), half_tokens)
    other_rows = pl.ds(pl.multiple_of(other_from, CHUNK), half_tokens)
    partner = {"c": 1 - at["c"]}

    def shared(rows, lanes, n):
        ref = red.at[rows, lanes]
        return pltpu.make_async_remote_copy(ref, ref, r_s.at[n], r_r.at[n], device_id=partner)

    x_part, y_part = slice(0, 512), slice(512, 768)
    in_other = [pl.ds(pl.multiple_of(other_from + i * CHUNK, CHUNK), CHUNK) for i in range(chunks)]
    over, back = (
        [shared(part(i), lanes, chunks * n + i) for n, lanes in enumerate((x_part, y_part)) for i in range(chunks)]
        for part in (in_array, lambda i: in_other[i])
    )

    def project(k, rows):
        return contract(red[rows, 256 * k : 256 * k + 256], cots[k, rows], 0, 0)

    half, quarter = 384, 192

    def block(h, ja, jb):
        a, b = ("x", "z") if h == 0 else ("z", "x")
        pos = {a: shift(a, ja), b: shift(b, jb)}
        return pos["z"] * RING + pos["x"]

    def hop(h, n, ja, jb, sub, along, d):
        axis = ("x", "z")[h] if along == 0 else ("z", "x")[h]
        start, size = (half * h, half) if sub is None else (half * h + quarter * sub, quarter)

        def ref(a, b):
            return g.at[block(h, a, b), start : start + size]

        src = ref(ja, jb)
        came = ref(ja - d, jb) if along == 0 else ref(ja, jb - d)
        peer = {axis: shift(axis, d)}
        out = pltpu.make_async_remote_copy(src, src, gs.at[h, n], gr.at[h, n], device_id=peer)
        arriving = pltpu.make_async_remote_copy(came, came, gs.at[h, n], gr.at[h, n], device_id=peer)
        return out, arriving

    hops = []
    for h in range(2):
        hops.append(hop(h, 0, 0, 0, None, 0, 1))
        hops.append(hop(h, 1, 0, 0, None, 0, -1))
        hops.append(hop(h, 2, -1, 0, 0, 0, 1))
        hops.append(hop(h, 3, 1, 0, 1, 0, -1))
        for j, ja in enumerate((0, -1, 1, 2)):
            hops.append(hop(h, 4 + 4 * j, ja, 0, None, 1, 1))
            hops.append(hop(h, 5 + 4 * j, ja, 0, None, 1, -1))
            hops.append(hop(h, 6 + 4 * j, ja, -1, 0, 1, 1))
            hops.append(hop(h, 7 + 4 * j, ja, 1, 1, 1, -1))

    def send(*ids):
        for n in ids:
            for h in range(2):
                hops[20 * h + n][0].start()

    def arrive(*ids):
        for n in ids:
            for h in range(2):
                hops[20 * h + n][1].wait_recv()

    send(0, 1, 4, 5)

    for c in b_copies[:2]:
        c.wait()
    x_copies[0].wait()
    for c in b_copies[2:] + y_copies + c_copies + m_copies:
        c.start()
    reduce_x(0)
    over[0].start()
    x_copies[1].wait()
    reduce_x(1)
    over[1].start()

    for c in c_copies[:2]:
        c.wait()
    for k in range(2):
        pacc[k] = project(k, mine_rows)

    def to_owners(ks, n):
        copies = []
        for slot, peer in enumerate(plane):
            owner = peer["z"] * RING + peer["x"]
            r = pl.ds(pl.multiple_of(owner * 16, 16), 16)
            copies.append(
                pltpu.make_async_remote_copy(
                    psend.at[ks, r, :], parr.at[ks, slot], a_s.at[n, slot], a_r.at[n, slot], device_id=peer
                )
            )
        return copies

    back[0].wait_recv()
    back[1].wait_recv()
    for k in range(2):
        psend[k] = ((pacc[k] + project(k, other_rows)) * factor).astype(BF16)
    first = to_owners(slice(0, 2), 0)
    for c in first:
        c.start()

    b_copies[2].wait()
    for c in y_copies:
        c.wait()
    red[mine_rows, 512:768] = jnp.dot(yb[...], bcat[:, 512:768], preferred_element_type=F32).astype(BF16)
    over[2].start()
    over[3].start()
    c_copies[2].wait()
    pacc[2] = project(2, mine_rows)
    arrive(0, 1)
    send(2, 3)
    back[2].wait_recv()
    back[3].wait_recv()
    psend[2] = ((pacc[2] + project(2, other_rows)) * factor).astype(BF16)
    second = to_owners(slice(2, 3), 1)
    for c in second:
        c.start()

    send(8, 9, 12, 13)
    for c in m_copies:
        c.wait()
    for c in first + second:
        c.wait_recv()
    mine = pl.ds(pl.multiple_of(me * 16, 16), 16)
    squares = []
    for k in range(3):
        total = psend[k, mine, :].astype(F32)
        for slot in range(len(PEERS)):
            total = total + parr[k, slot].astype(F32)
        first_moment = 0.9 * m1b[k] + 0.1 * total
        second_moment = 0.9 * m2b[k] + 0.1 * total * total
        direction = first_moment / (jnp.sqrt(second_moment) + 1e-08)
        m1o[k] = first_moment
        m2o[k] = second_moment
        for h in range(2):
            dg[h, k, at["z"], at["x"]] = direction[:, 128 * h : 128 * h + 128].astype(BF16)
        squares.append(direction * direction)

    def spread_copies(h, axis, where, sems):
        copies, arriving = [], []
        for i, (d, peer) in enumerate(zip(HOPS, ring[axis])):
            src, came = where(at[axis]), where(shift(axis, -d))
            copies.append(
                pltpu.make_async_remote_copy(src, src, sems[0].at[h, i], sems[1].at[h, i], device_id=peer)
            )
            arriving.append(
                pltpu.make_async_remote_copy(came, came, sems[0].at[h, i], sems[1].at[h, i], device_id=peer)
            )
        return copies, arriving

    near = [
        spread_copies(0, "x", lambda x: dg.at[0, :, at["z"], x], (d_s, d_r)),
        spread_copies(1, "z", lambda z: dg.at[1, :, z, at["x"]], (d_s, d_r)),
    ]
    far = [
        spread_copies(0, "z", lambda z: dg.at[0, :, z], (e_s, e_r)),
        spread_copies(1, "x", lambda x: dg.at[1, :, :, x], (e_s, e_r)),
    ]
    for n in (1, 0, 2):
        for copies, _ in near:
            copies[n].start()

    sums = [jnp.sum(v) for v in squares]
    lane = lax.broadcasted_iota(jnp.int32, (1, 128), 1)
    row = jnp.zeros((1, 128), F32)
    for k in range(3):
        row = row + jnp.where(lane == k, sums[k], 0.0)

    def sum_copies(held, peers, send_sems, recv_sems):
        return [
            pltpu.make_async_remote_copy(
                held.at[len(peers)], held.at[n], send_sems.at[n], recv_sems.at[n], device_id=peer
            )
            for n, peer in enumerate(peers)
        ]

    across = sum_copies(s1, heads, t_s, t_r)
    around = sum_copies(s2, plane, u_s, u_r)
    s1[len(TP_PEERS)] = row
    for c in across:
        c.start()

    arrive(2, 3)
    send(16, 17)
    arrive(4, 5)
    send(6, 7)

    for _, arriving in near:
        for c in arriving:
            c.wait_recv()
    for copies, _ in far:
        for c in copies:
            c.start()
    for c in across:
        c.wait_recv()
    s2[len(PEERS)] = jnp.sum(s1[...], axis=0)
    for c in around:
        c.start()

    arrive(8, 9, 12, 13)
    send(10, 11, 14, 15)
    arrive(16, 17)
    send(18, 19)

    for _, arriving in far:
        for c in arriving:
            c.wait_recv()
    for c in around:
        c.wait_recv()
    tot[...] = jnp.sum(s2[...], axis=0)
    arrive(6, 7, 10, 11, 14, 15, 18, 19)
    for out, _ in hops:
        out.wait_send()
    sent = over + first + second + across + around
    for copies, _ in near + far:
        sent = sent + copies
    for c in sent:
        c.wait_send()


def finish(
    entries, g, dg, tot, m1i, m2i, bcat, wf, wv, wo,
    nf_h, nv_h, no_h, cf_h, cv_h, co_h, m1_h, m2_h, sf_h, sv_h, so_h,
    nf, nv, no, cf, cv, co, sf, sv, so, dirs, dt, sem, csem,
):
    me = lax.axis_index("z") * RING + lax.axis_index("x")
    moments = [
        pltpu.make_async_copy(m1i, m1_h, sem.at[0]),
        pltpu.make_async_copy(m2i, m2_h, sem.at[1]),
    ]
    for c in moments:
        c.start()
    row = tot[...]
    lane = lax.broadcasted_iota(jnp.int32, (1, 128), 1)
    scale = [
        lax.rsqrt(jnp.sum(jnp.where(lane == k, row, 0.0), axis=1, keepdims=True) / entries + 1.0)
        for k in range(3)
    ]
    for k in range(3):
        for h in range(2):
            dirs[k, :, 128 * h : 128 * h + 128] = dg[h, k].reshape(256, 128)
    dt[...] = dirs[2].astype(F32).T.astype(BF16)
    outs = []
    for i in range(8):
        r = slice(256 * i, 256 * i + 256)
        for k, (copy, hbm) in enumerate(((cf, cf_h), (cv, cv_h))):
            full = jnp.dot(bcat[r, 256 * k : 256 * k + 256], dirs[k], preferred_element_type=F32)
            full = full * (0.01 * scale[k])
            for b in range(2):
                for p in range(2):
                    base = 256 * k + 128 * p
                    old = g[2 * i + b, base : base + 128, :].astype(F32)
                    part = full[128 * b : 128 * b + 128, 128 * p : 128 * p + 128]
                    copy[256 * i + 128 * b : 256 * i + 128 * b + 128, 128 * p : 128 * p + 128] = (
                        old - part
                    ).astype(BF16)
            outs.append(pltpu.make_async_copy(copy.at[r], hbm.at[r], csem.at[k, i]))
            outs[-1].start()
        full = contract(dt[...], bcat[r, 512:768], 1, 1) * (0.01 * scale[2])
        for b in range(2):
            old = g[2 * i + b, 512:768, :].astype(F32)
            co[:, 256 * i + 128 * b : 256 * i + 128 * b + 128] = (
                old - full[:, 128 * b : 128 * b + 128]
            ).astype(BF16)
        outs.append(pltpu.make_async_copy(co.at[:, r], co_h.at[:, r], csem.at[2, i]))
        outs[-1].start()
    rows = pl.ds(pl.multiple_of(me * 128, 128), 128)
    for k, (w, new, step) in enumerate(((wf, nf, sf), (wv, nv, sv))):
        full = jnp.dot(bcat[rows, 256 * k : 256 * k + 256], dirs[k], preferred_element_type=F32) * scale[k]
        step[...] = full
        new[...] = w[...] - 0.01 * full
    full = contract(dt[...], bcat[rows, 512:768], 1, 1) * scale[2]
    so[...] = full
    no[...] = wo[...] - 0.01 * full
    own = [
        pltpu.make_async_copy(s, d, sem.at[2 + i])
        for i, (s, d) in enumerate(
            ((nf, nf_h), (nv, nv_h), (no, no_h), (sf, sf_h), (sv, sv_h), (so, so_h))
        )
    ]
    for c in own:
        c.start()
    for c in moments + own + outs:
        c.wait()


def on_device(x, fc, vc, go, y, wf, wv, wo, bases, m1, m2):
    tokens = x.shape[0]
    hbm = pl.BlockSpec(memory_space=pltpu.HBM)
    vmem = pl.BlockSpec(memory_space=pltpu.VMEM)
    dma = pltpu.SemaphoreType.DMA
    m1, m2 = (jnp.transpose(m, (1, 0, 2)) for m in (m1, m2))
    args = [
        pltpu.with_memory_space_constraint(a, pltpu.HBM) for a in (x, y, fc, vc, go, wf, wv, wo, bases, m1, m2)
    ]
    held = pl.pallas_call(
        exchange,
        name="exchange",
        out_shape=[
            pltpu.VMEM((16, 768, 128), BF16),
            pltpu.VMEM((2, 3, 4, 4, 16, 128), BF16),
            pltpu.VMEM((1, 128), F32),
            pltpu.VMEM((3, 16, 256), F32),
            pltpu.VMEM((3, 16, 256), F32),
            pltpu.VMEM((2048, 768), BF16),
            pltpu.VMEM((128, 256), F32),
            pltpu.VMEM((128, 256), F32),
            pltpu.VMEM((256, 128), F32),
        ],
        in_specs=[hbm] * 11,
        out_specs=[vmem] * 9,
        scratch_shapes=[
            pltpu.VMEM((tokens // 2, 2048), BF16),
            pltpu.VMEM((tokens // 2, 2048), BF16),
            pltpu.VMEM((3, tokens, 256), BF16),
            pltpu.VMEM((tokens, 768), BF16),
            pltpu.VMEM((3, 16, 256), F32),
            pltpu.VMEM((3, 16, 256), F32),
            pltpu.VMEM((3, 256, 256), F32),
            pltpu.VMEM((3, 256, 256), BF16),
            pltpu.VMEM((3, 15, 16, 256), BF16),
            pltpu.VMEM((8, 1, 128), F32),
            pltpu.VMEM((16, 1, 128), F32),
            dma((3,)),
            dma((3,)),
            dma((2,)),
            dma((2,)),
            dma((2,)),
            dma((3,)),
            dma((4,)),
            dma((4,)),
            dma((2, 20)),
            dma((2, 20)),
            dma((2, 15)),
            dma((2, 15)),
            dma((2, 3)),
            dma((2, 3)),
            dma((2, 3)),
            dma((2, 3)),
            dma((7,)),
            dma((7,)),
            dma((15,)),
            dma((15,)),
        ],
        compiler_params=pltpu.CompilerParams(
            collective_id=0, has_side_effects=True, vmem_limit_bytes=40 * MiB
        ),
    )(*args)
    shapes = [
        ((128, 256), F32),
        ((128, 256), F32),
        ((256, 128), F32),
        ((2048, 256), BF16),
        ((2048, 256), BF16),
        ((256, 2048), BF16),
        ((3, 16, 256), F32),
        ((3, 16, 256), F32),
        ((128, 256), F32),
        ((128, 256), F32),
        ((256, 128), F32),
    ]
    outs = pl.pallas_call(
        functools.partial(finish, float(256 * 2048)),
        name="finish",
        out_shape=[jax.ShapeDtypeStruct(*s) for s in shapes],
        in_specs=[vmem] * 9,
        out_specs=[hbm] * 11,
        scratch_shapes=[
            *(pltpu.VMEM(*s) for s in shapes[:6]),
            *(pltpu.VMEM(*s) for s in shapes[8:]),
            pltpu.VMEM((3, 256, 256), BF16),
            pltpu.VMEM((256, 256), BF16),
            dma((8,)),
            dma((3, 8)),
        ],
        compiler_params=pltpu.CompilerParams(vmem_limit_bytes=24 * MiB),
    )(*held)
    outs = list(outs)
    outs[6], outs[7] = (jnp.transpose(m, (1, 0, 2)) for m in outs[6:8])
    return tuple(outs)


def solution(mesh):
    torus = Mesh(mesh.devices.reshape(4, 4, 4, 2), ("z", "x", "y", "c"))
    rows, heads, both = P(FS, None), P(FS, TP), P(FS, None, TP)
    turned = P(TP, FS)
    return jax.shard_map(
        on_device,
        mesh=torus,
        in_specs=(rows, heads, heads, heads, rows, heads, heads, turned, P(), both, both),
        out_specs=(
            heads, heads, turned, P(None, TP), P(None, TP), P(TP, None), both, both, heads, heads, turned,
        ),
        check_vma=False,
    )
```
